32 devices in a mesh: sp: 8 (over z, x), tp: 4 (over y, core).
Axes of the slice: x: 2, y: 2, z: 4, core: 2. Of those that a mesh axis runs over, the one named last changes fastest.
Arguments:
- stream: bfloat16 [4096, 2048], P('sp', 'tp'), may hold values from -6 to 6
- norm_gain: float32 [2, 2048], replicated, may hold values from 0.1 to 1.9
- w_value: bfloat16 [2, 2048, 2048], P(None, 'sp', 'tp'), may hold values from -0.125 to 0.125
- w_inner: bfloat16 [2, 2048, 2048], P(None, 'sp', 'tp'), may hold values from -0.125 to 0.125
- w_outer: bfloat16 [2, 2048, 2048], P(None, 'sp', 'tp'), may hold values from -0.125 to 0.125
- conv_taps: float32 [2, 3, 2048], P(None, None, 'tp'), may hold values from -3 to 3
- w_output: bfloat16 [2, 2048, 2048], P(None, 'tp', 'sp'), may hold values from -0.125 to 0.125
Outputs:
- result: bfloat16 [4096, 2048], P('sp', 'tp')
The draws below stay inside these ranges and needn't reach their ends.
All inputs are finite; a program needn't handle non-finite values.
Results may differ from the reference program's by a relative error of at most 0.02.
Values may be sent and summed in bfloat16 or wider, within the bound.
No kernel may reach another device: no remote copies, remote signals or barrier semaphores. Data moves between devices by JAX's collectives and lax.ppermute only.
A program may use at most 64 MiB of HBM per device.

```python
import jax
import jax.numpy as jnp
from jax import lax

D = 2048
LAYERS = 2
TAPS = 3
TOKENS = 4096
N_TP = 4


def steps_of(stream_key, dims, shards, smallest, largest):
    level, own = 1.0, jax.random.fold_in(stream_key, 6)
    for dim, shards_of in shards:
        heights = jnp.exp(jax.random.uniform(jax.random.fold_in(own, dim), (shards_of,), jnp.float32, smallest / len(shards), largest / len(shards)))
        level = level * jnp.repeat(heights, dims[dim] // shards_of).reshape([-1 if axis == dim else 1 for axis in range(len(dims))])
    return level


def bell_draw(own_key, shape, scale, limit, pieces=(), kind=jnp.bfloat16):
    factor_of = steps_of(own_key, shape, pieces, -0.22, 0.18) if pieces else 1.0
    result = jax.random.normal(own_key, shape, jnp.float32) * scale * factor_of
    return jnp.minimum(jnp.maximum(result, -limit), limit).astype(kind)


def setup_inputs(seed: int = 0) -> dict:
    seeds = jax.random.split(jax.random.key(seed), 8)
    return {
        "stream": bell_draw(seeds[0], (TOKENS, D), 1.0, 6.0, ((0, 8), (1, 4))),
        "norm_gain": jnp.clip(1.0 + 0.18 * jax.random.normal(seeds[1], (LAYERS, D), jnp.float32), 0.1, 1.9),
        "w_value": bell_draw(seeds[2], (LAYERS, D, D), D ** -0.5, 0.125, ((1, 8), (2, 4))),
        "w_inner": bell_draw(seeds[3], (LAYERS, D, D), D ** -0.5, 0.125, ((1, 8), (2, 4))),
        "w_outer": bell_draw(seeds[4], (LAYERS, D, D), D ** -0.5, 0.125, ((1, 8), (2, 4))),
        "conv_taps": bell_draw(seeds[5], (LAYERS, TAPS, D), 0.6, 3.0, ((2, 4),), jnp.float32),
        "w_output": bell_draw(seeds[6], (LAYERS, D, D), D ** -0.5, 0.125, ((1, 4), (2, 8))),
    }


EPSILON = 1e-06

def one_layer(stream_now, gain, weight_value, weight_inner, weight_outer, taps, weight_output):
    stream_float = stream_now.astype(jnp.float32)
    scale = lax.rsqrt(lax.optimization_barrier(jnp.mean(stream_float * stream_float, axis=-1, keepdims=True)) + EPSILON)
    normed = (stream_float * scale * gain).astype(jnp.bfloat16)
    value_proj = jnp.dot(normed, weight_value, preferred_element_type=jnp.float32)
    inner_gate = jnp.dot(normed, weight_inner, preferred_element_type=jnp.float32)
    outer_gate = jnp.dot(normed, weight_outer, preferred_element_type=jnp.float32)
    mixed = (inner_gate * value_proj).astype(jnp.bfloat16)
    row_count = mixed.shape[0]
    padded = jnp.pad(mixed.astype(jnp.float32), ((2, 0), (0, 0)))
    convolved = taps[0] * padded[0:row_count] + taps[1] * padded[1:row_count + 1] + taps[2] * padded[2:]
    gated = (outer_gate * convolved).astype(jnp.bfloat16)
    block_width = gated.shape[1] // N_TP
    summed = jnp.zeros((row_count, gated.shape[1]), jnp.float32)
    for block_index in range(N_TP):
        low = block_index * block_width
        partial_value = jnp.dot(gated[:, low:low + block_width], weight_output[low:low + block_width], preferred_element_type=jnp.float32).astype(jnp.bfloat16)
        partial_value = lax.optimization_barrier(partial_value)
        summed = summed + partial_value.astype(jnp.float32)
    return (stream_float + summed).astype(jnp.bfloat16)

def reference(stream, norm_gain, w_value, w_inner, w_outer, conv_taps, w_output):
    stream_now = stream
    for layer_index in range(LAYERS):
        stream_now = one_layer(stream_now, norm_gain[layer_index], w_value[layer_index], w_inner[layer_index], w_outer[layer_index], conv_taps[layer_index], w_output[layer_index])
    return stream_now
```

```python
import jax
import jax.numpy as jnp
from jax import lax
from jax.sharding import PartitionSpec as P

EPSILON = 1e-06
AXES = ("sp", "tp")


class Grid:
    def __init__(self):
        self.n_sp, self.n_tp = lax.axis_size("sp"), lax.axis_size("tp")
        self.planes, self.rows = self.n_sp // 2, self.n_tp // 2
        sp, tp = lax.axis_index("sp"), lax.axis_index("tp")
        self.plane, self.column = sp // 2, sp % 2
        self.row, self.core = tp // 2, tp % 2

    def flat(self, plane, column, row, core):
        return (plane * 2 + column) * self.n_tp + row * 2 + core

    def send(self, block, target):
        pairs = []
        for plane in range(self.planes):
            for column in range(2):
                for row in range(self.rows):
                    for core in range(2):
                        to = target(plane, column, row, core)
                        if to is not None:
                            pairs.append((self.flat(plane, column, row, core), self.flat(*to)))
        return lax.ppermute(block, AXES, pairs)

    def across(self, block):
        return self.send(
            block, lambda p, x, y, c: (p, x, y, c) if x == c else (p, 1 - x, y, 1 - c)
        )

    def along(self, block):
        return self.send(block, lambda p, x, y, c: ((p + 1) % self.planes, x, y, c))

    def other_core(self, block):
        return self.send(block, lambda p, x, y, c: (p, x, y, 1 - c))

    def halo(self, block):
        def target(p, x, y, c):
            if c == 0:
                return (p, x, y, 1)
            return (p + 1, x, y, 0) if p + 1 < self.planes else None

        return self.send(block, target)

    def gather(self, block):
        pieces = []
        for a in range(self.rows):
            for b in range(2):
                piece = self.send(block, lambda p, x, y, c: (p, c ^ b, (y + a) % self.rows, x))
                owner = ((self.row - a) % self.rows) * 2 + (self.column ^ b)
                pieces.append((owner, piece))
        return pieces

    def scatter(self, terms, width):
        pieces = []
        for a in range(self.rows):
            for b in range(2):
                owner = ((self.row - a) % self.rows) * 2 + (self.column ^ b)
                part = lax.dynamic_slice_in_dim(terms, owner * width, width, 1)
                pieces.append(
                    self.send(part, lambda p, x, y, c: (p, c, (y - a) % self.rows, x ^ b))
                )
        return pieces


def ring(grid, shard):
    held = grid.across(shard)
    slots = [(held, grid.other_core(held))]
    for _ in range(grid.planes - 1):
        held = grid.along(held)
        slots.append((held, grid.other_core(held)))
    return slots


def on_device(stream, norm_gain, w_value, w_inner, w_outer, conv_taps, w_output):
    grid = Grid()
    layers = norm_gain.shape[0]
    tokens, width = stream.shape
    depth = width * grid.n_tp
    rows_in = w_value.shape[1]
    columns_out = w_output.shape[2]
    held_in, held_out = [], []
    for layer in range(layers):
        joined = jnp.stack([w_value[layer], w_inner[layer], w_outer[layer]])
        held_in.append(ring(grid, joined))
        held_out.append(ring(grid, w_output[layer]))
    taps_mine = grid.send(conv_taps, lambda p, x, y, c: (p, c, y, x))

    stream_now = stream
    for layer in range(layers):
        full = jnp.zeros((tokens, depth), jnp.bfloat16)
        for owner, piece in grid.gather(stream_now):
            full = lax.dynamic_update_slice_in_dim(full, piece, owner * width, 1)
        row_float = full.astype(jnp.float32)
        scale = lax.rsqrt(jnp.mean(row_float * row_float, axis=-1, keepdims=True) + EPSILON)
        normed = (row_float * scale * norm_gain[layer]).astype(jnp.bfloat16)
        parts = None
        for step, pair in enumerate(held_in[layer]):
            block = (grid.plane - step) % grid.planes
            for index, weights in enumerate(pair):
                start = (block * 2 + (grid.core ^ index)) * rows_in
                part = lax.dynamic_slice_in_dim(normed, start, rows_in, 1)
                products = [
                    jnp.dot(part, weights[k], preferred_element_type=jnp.float32) for k in range(3)
                ]
                parts = products if parts is None else [u + v for u, v in zip(parts, products)]
        value, inner, outer = parts
        mixed = (inner * value).astype(jnp.bfloat16)
        before = grid.halo(mixed[tokens - 2 :])
        padded = jnp.concatenate([before, mixed], axis=0).astype(jnp.float32)
        taps = taps_mine[layer]
        convolved = (
            taps[0] * padded[0:tokens]
            + taps[1] * padded[1 : tokens + 1]
            + taps[2] * padded[2:]
        )
        gated = (outer * convolved).astype(jnp.bfloat16)
        terms = jnp.zeros((tokens, depth), jnp.bfloat16)
        for step, pair in enumerate(held_out[layer]):
            block = (grid.plane - step) % grid.planes
            for index, weights in enumerate(pair):
                start = (block * 2 + (grid.core ^ index)) * columns_out
                product = jnp.dot(gated, weights, preferred_element_type=jnp.float32)
                terms = lax.dynamic_update_slice_in_dim(
                    terms, product.astype(jnp.bfloat16), start, 1
                )
        summed = stream_now.astype(jnp.float32)
        for piece in grid.scatter(terms, width):
            summed = summed + piece.astype(jnp.float32)
        stream_now = summed.astype(jnp.bfloat16)
    return stream_now


def solution(mesh):
    in_specs = (
        P("sp", "tp"),
        P(),
        P(None, "sp", "tp"),
        P(None, "sp", "tp"),
        P(None, "sp", "tp"),
        P(None, None, "tp"),
        P(None, "tp", "sp"),
    )
    return jax.shard_map(
        on_device, mesh=mesh, in_specs=in_specs, out_specs=P("sp", "tp"), check_vma=False
    )
```
